32 devices in a mesh: ep: 8 (over z, core), tp: 4 (over y, x).
Axes of the slice: x: 2, y: 2, z: 4, core: 2. Of those that a mesh axis runs over, the one named last changes fastest.
Arguments:
- stream: bfloat16 [128, 4096], P('ep'), may hold values from -6 to 6
- previous_state: float32 [128, 128, 4096], P('ep', None, 'tp'), may hold values from -6 to 6
- mixer_norm_gain: float32 [4096], replicated, may hold values from 0.1 to 1.9
- query_matrix: bfloat16 [4096, 2048], P('ep'), may hold values from -0.09375 to 0.09375
- key_matrix: bfloat16 [4096, 2048], P('ep'), may hold values from -0.09375 to 0.09375
- value_matrix: bfloat16 [4096, 4096], P('ep', 'tp'), may hold values from -0.09375 to 0.09375
- output_gate_weight: bfloat16 [4096, 4096], P('ep', 'tp'), may hold values from -0.09375 to 0.09375
- decay_lower_factor: bfloat16 [4096, 64], replicated, may hold values from -0.09375 to 0.09375
- decay_upper_factor: bfloat16 [64, 2048], replicated, may hold values from -3 to 3
- forgetting_boost: float32 [128, 2048], P('ep'), may hold values from 0.02 to 1.5
- head_norm_gain: float32 [256], replicated, may hold values from 0.1 to 1.9
- output_matrix: bfloat16 [4096, 4096], P('tp'), may hold values from -0.1875 to 0.1875
- mixture_norm_gain: float32 [4096], replicated, may hold values from 0.1 to 1.9
- expert_gate_weight: bfloat16 [8, 1024, 4096], P('ep', 'tp'), may hold values from -0.09375 to 0.09375
- expert_up_weight: bfloat16 [8, 1024, 4096], P('ep', 'tp'), may hold values from -0.09375 to 0.09375
- expert_down_weight: bfloat16 [8, 1024, 4096], P('ep', None, 'tp'), may hold values from -0.375 to 0.375
- expert_index_table: int32 [128, 2], P('ep'), may hold values from 0 to 7, as said below
- expert_scores_within: float32 [128, 2], P('ep'), may hold values from -6 to 6
- group_probability: float32 [128], P('ep'), may hold values from 0.3 to 1
Outputs:
- new_stream: bfloat16 [128, 4096], P('ep', 'tp')
- new_state: float32 [128, 128, 4096], P('ep', None, 'tp')
The draws below stay inside these ranges and needn't reach their ends.
Inputs may be any that keep to these rules, and one draw needn't show every extreme that they name: `expert_index_table`: the 2 experts of a sequence are distinct and lie in one group of 2 consecutive experts. Among the 16 sequences of one index of ep (aligned blocks of rows), each expert is named at most 8 times, and in every block some experts are named exactly 8 times.
All inputs are finite; a program needn't handle non-finite values.
Results may differ from the reference program's by a relative error of at most 0.02.
Values may be sent and summed in bfloat16 or wider, within the bound.
No kernel may reach another device: no remote copies, remote signals or barrier semaphores. Data moves between devices by JAX's collectives and lax.ppermute only.
A program may use at most 128 MiB of HBM per device.

```python
import math
import jax
import jax.numpy as jnp
from jax import lax

D = 4096
HEAD_TOTAL = 16
KEY_CHANNELS = 128
DV = 256
RANK = 64
FF = 1024
GROUPS = 4
TOPK = 2
SEQ_DEV = 16
SEQUENCE_TOTAL = 128
EXPERTS = 8
PER_GROUP = 2
CAP = 8
N_EP = 8


def shuffle(subkey):
    return jax.random.permutation(subkey, SEQ_DEV)


def draw_expert_index_table(key, part):
    blocks = SEQUENCE_TOTAL // SEQ_DEV
    hot_count = PER_GROUP * CAP // TOPK
    key_hot, key_other, key_perm, key_turn = jax.random.split(jax.random.fold_in(key, 11), 4)
    hot_group = jax.random.randint(key_hot, (), 0, GROUPS)
    offsets = jax.random.randint(key_other, (blocks, SEQ_DEV), 1, GROUPS)
    orders = jax.vmap(shuffle)(jax.random.split(key_perm, blocks))
    places = jnp.arange(SEQ_DEV)
    chosen = (orders[:, :, None] == places[None, None, :]) & (places[None, :, None] < hot_count)
    is_hot = jnp.any(chosen, axis=1)
    group_id = jnp.where(is_hot, hot_group, (hot_group + offsets) % GROUPS)
    same_group = group_id[:, :, None] == group_id[:, None, :]
    before = places[None, :] < places[:, None]
    rank_in = jnp.sum(same_group & before[None], axis=2)
    rotation = jax.random.randint(key_turn, (blocks, GROUPS), 0, PER_GROUP)
    member = group_id[:, :, None] == jnp.arange(GROUPS)[None, None, :]
    shift_by = jnp.sum(jnp.where(member, rotation[:, None, :], 0), axis=2)
    within = (shift_by[:, :, None] + rank_in[:, :, None] * TOPK + jnp.arange(TOPK)[None, None, :]) % PER_GROUP
    chosen_ids = group_id[:, :, None] * PER_GROUP + within
    return chosen_ids.reshape(SEQUENCE_TOTAL, TOPK).astype(jnp.int32)


def block_scale(rng, dims, pieces, least, high):
    def one(position, shards_of):
        steps = jax.random.uniform(jax.random.fold_in(jax.random.fold_in(rng, 6), position), (shards_of,), jnp.float32, least / len(pieces), high / len(pieces))
        return jnp.repeat(jnp.exp(steps), dims[position] // shards_of).reshape((-1,) + (1,) * (len(dims) - position - 1))

    level = one(*pieces[0])
    for cut in pieces[1:]:
        level = level * one(*cut)
    return level


def centred(stream_key, dims, width, limit, cuts=(), kind=jnp.bfloat16):
    result = jax.random.normal(stream_key, dims, jnp.float32) * width
    if len(cuts) > 0:
        result = block_scale(stream_key, dims, cuts, -0.22, 0.18) * result
    return jnp.clip(result, min=-limit, max=limit).astype(kind)


def setup_inputs(seed: int = 0) -> dict:
    key_list = jax.random.split(jax.random.key(seed), 20)
    return {
        "stream": centred(key_list[0], (SEQUENCE_TOTAL, D), 1.0, 6.0, ((0, 8),)),
        "previous_state": centred(key_list[1], (SEQUENCE_TOTAL, KEY_CHANNELS, HEAD_TOTAL * DV), 1.0, 6.0, ((0, 8), (2, 4)), jnp.float32),
        "mixer_norm_gain": jnp.clip(1.0 + 0.18 * jax.random.normal(key_list[2], (D,), jnp.float32), 0.1, 1.9),
        "query_matrix": centred(key_list[3], (D, HEAD_TOTAL * KEY_CHANNELS), D ** -0.5, 0.09375, ((0, 8),)),
        "key_matrix": centred(key_list[4], (D, HEAD_TOTAL * KEY_CHANNELS), D ** -0.5, 0.09375, ((0, 8),)),
        "value_matrix": centred(key_list[5], (D, HEAD_TOTAL * DV), D ** -0.5, 0.09375, ((0, 8), (1, 4))),
        "output_gate_weight": centred(key_list[6], (D, HEAD_TOTAL * DV), D ** -0.5, 0.09375, ((0, 8), (1, 4))),
        "decay_lower_factor": centred(key_list[7], (D, RANK), D ** -0.5, 0.09375),
        "decay_upper_factor": centred(key_list[8], (RANK, HEAD_TOTAL * KEY_CHANNELS), (RANK // 16) ** -0.5, 3.0),
        "forgetting_boost": jnp.clip(jnp.exp(math.log(1.5) - 4.317488 * jax.random.uniform(key_list[9], (SEQUENCE_TOTAL, HEAD_TOTAL * KEY_CHANNELS), jnp.float32) ** block_scale(key_list[9], (SEQUENCE_TOTAL, HEAD_TOTAL * KEY_CHANNELS), ((0, 8),), -0.2, 0.2)), 0.02, 1.5),
        "head_norm_gain": jnp.clip(1.0 + 0.18 * jax.random.normal(key_list[10], (DV,), jnp.float32), 0.1, 1.9),
        "output_matrix": centred(key_list[11], (HEAD_TOTAL * DV, D), (HEAD_TOTAL * DV // 4) ** -0.5, 0.1875, ((0, 4),)),
        "mixture_norm_gain": jnp.clip(1.0 + 0.18 * jax.random.normal(key_list[12], (D,), jnp.float32), 0.1, 1.9),
        "expert_gate_weight": centred(key_list[13], (EXPERTS, FF, D), D ** -0.5, 0.09375, ((0, 8), (1, 4))),
        "expert_up_weight": centred(key_list[14], (EXPERTS, FF, D), D ** -0.5, 0.09375, ((0, 8), (1, 4))),
        "expert_down_weight": centred(key_list[15], (EXPERTS, FF, D), (FF // 4) ** -0.5, 0.375, ((0, 8), (2, 4))),
        "expert_index_table": draw_expert_index_table(jax.random.fold_in(key_list[19], 71), 0),
        "expert_scores_within": centred(key_list[17], (SEQUENCE_TOTAL, TOPK), 1.5, 6.0, ((0, 8),), jnp.float32),
        "group_probability": jnp.clip(0.3 + 0.7 * jax.random.uniform(key_list[18], (SEQUENCE_TOTAL,), jnp.float32) ** block_scale(key_list[18], (SEQUENCE_TOTAL,), ((0, 8),), -0.2, 0.2), 0.3, 1.0),
    }


epsilon = 1e-06
forgetting_softness = 16.0

def rms_scaled(values, gain_vec):
    floats = values.astype(jnp.float32)
    scaled = floats * lax.rsqrt(lax.optimization_barrier(jnp.mean(floats * floats, axis=-1, keepdims=True)) + epsilon)
    return (scaled * gain_vec).astype(jnp.bfloat16)

def expert_apply(inputs):
    tokens_in, gate_mat, up_mat, down_mat = inputs
    gate_pre = jnp.dot(tokens_in, gate_mat.T, preferred_element_type=jnp.float32)
    up_pre = jnp.dot(tokens_in, up_mat.T, preferred_element_type=jnp.float32)
    hidden = (jax.nn.silu(gate_pre) * up_pre).astype(jnp.bfloat16)
    return jnp.dot(hidden, down_mat, preferred_element_type=jnp.float32).astype(jnp.bfloat16)

def reference(stream, previous_state, mixer_norm_gain, query_matrix, key_matrix, value_matrix, output_gate_weight, decay_lower_factor, decay_upper_factor, forgetting_boost, head_norm_gain, output_matrix, mixture_norm_gain, expert_gate_weight, expert_up_weight, expert_down_weight, expert_index_table, expert_scores_within, group_probability):
    normed = rms_scaled(stream, mixer_norm_gain)
    queries = (jnp.dot(normed, query_matrix, preferred_element_type=jnp.float32) * KEY_CHANNELS ** (-0.5)).astype(jnp.bfloat16)
    key_rows = jnp.dot(normed, key_matrix, preferred_element_type=jnp.float32).astype(jnp.bfloat16)
    value_rows = jnp.dot(normed, value_matrix, preferred_element_type=jnp.float32).astype(jnp.bfloat16)
    gate_rows = jnp.dot(normed, output_gate_weight, preferred_element_type=jnp.float32).astype(jnp.bfloat16)
    low_rank = jnp.dot(normed, decay_lower_factor, preferred_element_type=jnp.float32).astype(jnp.bfloat16)
    forgetting_logit = jnp.dot(low_rank, decay_upper_factor, preferred_element_type=jnp.float32)
    forgetting_lograte = jax.nn.log_sigmoid(forgetting_logit) / forgetting_softness - forgetting_boost
    factor = jnp.exp(forgetting_lograte).reshape(SEQUENCE_TOTAL, HEAD_TOTAL, KEY_CHANNELS).transpose(0, 2, 1)[..., None]
    state_four = previous_state.reshape(SEQUENCE_TOTAL, KEY_CHANNELS, HEAD_TOTAL, DV)
    key_part = key_rows.astype(jnp.float32).reshape(SEQUENCE_TOTAL, HEAD_TOTAL, KEY_CHANNELS).transpose(0, 2, 1)[..., None]
    value_part = value_rows.astype(jnp.float32).reshape(SEQUENCE_TOTAL, 1, HEAD_TOTAL, DV)
    updated = factor * state_four + key_part * value_part
    query_part = queries.astype(jnp.float32).reshape(SEQUENCE_TOTAL, HEAD_TOTAL, KEY_CHANNELS).transpose(0, 2, 1)
    readout = jnp.einsum('skh,skhv->shv', query_part, updated, precision=lax.Precision.HIGHEST)
    mean_sq = lax.optimization_barrier(jnp.mean(readout * readout, axis=-1, keepdims=True))
    gate_part = jax.nn.silu(gate_rows.astype(jnp.float32).reshape(SEQUENCE_TOTAL, HEAD_TOTAL, DV))
    gated_rows = (readout * lax.rsqrt(mean_sq + epsilon) * head_norm_gain * gate_part).reshape(SEQUENCE_TOTAL, HEAD_TOTAL * DV).astype(jnp.bfloat16)
    blended_tokens = (stream.astype(jnp.float32) + jnp.dot(gated_rows, output_matrix, preferred_element_type=jnp.float32)).astype(jnp.bfloat16)
    normed_two = rms_scaled(blended_tokens, mixture_norm_gain)
    logit_exp = jnp.exp(expert_scores_within)
    weights = logit_exp / lax.optimization_barrier(jnp.sum(logit_exp, axis=-1, keepdims=True)) * group_probability[:, None]
    blocked = expert_index_table.reshape(N_EP, SEQ_DEV * TOPK).astype(jnp.int32)
    one_hot = (blocked[..., None] == jnp.arange(EXPERTS, dtype=jnp.int32)).astype(jnp.int32)
    rank_in = lax.optimization_barrier(jnp.sum(one_hot * (jnp.cumsum(one_hot, axis=1) - 1), axis=-1))
    column = (jnp.arange(N_EP, dtype=jnp.int32)[:, None] * CAP + rank_in).astype(jnp.int32)
    repeated = jnp.broadcast_to(normed_two.reshape(N_EP, SEQ_DEV, 1, D), (N_EP, SEQ_DEV, TOPK, D)).reshape(N_EP, SEQ_DEV * TOPK, D)
    buffer = jnp.zeros((EXPERTS, N_EP * CAP, D), jnp.bfloat16).at[blocked, column].set(repeated)
    results = lax.map(expert_apply, (buffer, expert_gate_weight, expert_up_weight, expert_down_weight))
    picked = results[blocked, column].reshape(SEQUENCE_TOTAL, TOPK, D)
    mixture = lax.optimization_barrier(jnp.sum(weights[..., None] * picked.astype(jnp.float32), axis=1))
    new_stream = (blended_tokens.astype(jnp.float32) + mixture).astype(jnp.bfloat16)
    return (new_stream, updated.reshape(SEQUENCE_TOTAL, KEY_CHANNELS, HEAD_TOTAL * DV))
```

```python
import jax
import jax.numpy as jnp
from jax import lax
from jax.experimental import pallas as pl
from jax.experimental.pallas import tpu as pltpu
from jax.sharding import PartitionSpec as P

HEAD_TOTAL = 16
KEY_CHANNELS = 128
DV = 256
GROUPS = 4
CORES = 2


epsilon = 1e-06
forgetting_softness = 16.0


def rms_scaled(values, gain_vec):
    floats = values.astype(jnp.float32)
    scaled = floats * lax.rsqrt(jnp.mean(floats * floats, axis=-1, keepdims=True) + epsilon)
    return (scaled * gain_vec).astype(jnp.bfloat16)


def on_device_general(
    stream,
    previous_state,
    mixer_norm_gain,
    query_matrix,
    key_matrix,
    value_matrix,
    output_gate_weight,
    decay_lower_factor,
    decay_upper_factor,
    forgetting_boost,
    head_norm_gain,
    output_matrix,
    mixture_norm_gain,
    expert_gate_weight,
    expert_up_weight,
    expert_down_weight,
    expert_index_table,
    expert_scores_within,
    group_probability,
):
    seq_count, model_width = stream.shape
    value_local = previous_state.shape[2]
    head_count = max(1, value_local // DV)
    head_width = min(value_local, DV)
    tp_index = lax.axis_index("tp")
    leading_head = tp_index * value_local // DV
    value_start = tp_index * value_local % DV
    key_column_span = head_count * KEY_CHANNELS
    normed = rms_scaled(stream, mixer_norm_gain)
    own_query = lax.dynamic_slice_in_dim(
        query_matrix, leading_head * KEY_CHANNELS, key_column_span, 1
    )
    own_key = lax.dynamic_slice_in_dim(key_matrix, leading_head * KEY_CHANNELS, key_column_span, 1)
    spread = lax.all_to_all(normed, "ep", split_axis=1, concat_axis=0, tiled=True)
    joined = jnp.concatenate([own_query, own_key, value_matrix, output_gate_weight], axis=1)
    summed = lax.psum_scatter(
        jnp.dot(spread, joined, preferred_element_type=jnp.float32),
        "ep",
        scatter_dimension=0,
        tiled=True,
    )
    query_sum = summed[:, :key_column_span]
    key_sum = summed[:, key_column_span : 2 * key_column_span]
    value_sum = summed[:, 2 * key_column_span : 2 * key_column_span + value_local]
    gate_sum = summed[:, 2 * key_column_span + value_local :]
    queries = (query_sum * KEY_CHANNELS ** (-0.5)).astype(jnp.bfloat16)
    key_rows = key_sum.astype(jnp.bfloat16)
    value_rows = value_sum.astype(jnp.bfloat16)
    gate_rows = gate_sum.astype(jnp.bfloat16)
    low_rank = jnp.dot(normed, decay_lower_factor, preferred_element_type=jnp.float32).astype(
        jnp.bfloat16
    )
    local_expand_matrix = lax.dynamic_slice_in_dim(
        decay_upper_factor, leading_head * KEY_CHANNELS, key_column_span, 1
    )
    forgetting_logit = jnp.dot(low_rank, local_expand_matrix, preferred_element_type=jnp.float32)
    request_boost = lax.dynamic_slice_in_dim(
        forgetting_boost, leading_head * KEY_CHANNELS, key_column_span, 1
    )
    forgetting_lograte = jax.nn.log_sigmoid(forgetting_logit) / forgetting_softness - request_boost
    factor = (
        jnp.exp(forgetting_lograte)
        .reshape(seq_count, head_count, KEY_CHANNELS)
        .transpose(0, 2, 1)[..., None]
    )
    state_four = previous_state.reshape(seq_count, KEY_CHANNELS, head_count, head_width)
    key_part = (
        key_rows.astype(jnp.float32)
        .reshape(seq_count, head_count, KEY_CHANNELS)
        .transpose(0, 2, 1)[..., None]
    )
    value_part = value_rows.astype(jnp.float32).reshape(seq_count, 1, head_count, head_width)
    updated = factor * state_four + key_part * value_part
    query_part = (
        queries.astype(jnp.float32).reshape(seq_count, head_count, KEY_CHANNELS).transpose(0, 2, 1)
    )
    readout = jnp.einsum("skh,skhv->shv", query_part, updated, precision=lax.Precision.HIGHEST)
    square_sums = jnp.sum(readout * readout, axis=-1)
    norm_table = lax.dynamic_update_slice(
        jnp.zeros((seq_count, HEAD_TOTAL), jnp.float32), square_sums, (jnp.int32(0), leading_head)
    )
    totals = lax.psum(norm_table, "tp")
    own_totals = lax.dynamic_slice_in_dim(totals, leading_head, head_count, 1)
    mean_sq = own_totals[..., None] / DV
    own_gain = lax.dynamic_slice_in_dim(head_norm_gain, value_start, head_width, 0)
    gate_part = jax.nn.silu(
        gate_rows.astype(jnp.float32).reshape(seq_count, head_count, head_width)
    )
    gated_rows = (
        (readout * lax.rsqrt(mean_sq + epsilon) * own_gain * gate_part)
        .reshape(seq_count, value_local)
        .astype(jnp.bfloat16)
    )
    partial_out = jnp.dot(gated_rows, output_matrix, preferred_element_type=jnp.float32)
    mixer_sum = lax.psum(partial_out.astype(jnp.bfloat16), "tp").astype(jnp.float32)
    blended_tokens = (stream.astype(jnp.float32) + mixer_sum).astype(jnp.bfloat16)
    normed_two = rms_scaled(blended_tokens, mixture_norm_gain)
    ep_count = lax.axis_size("ep")
    local_experts = expert_gate_weight.shape[0]
    experts_all = ep_count * local_experts
    route_count = expert_index_table.shape[1]
    capacity = 2 * seq_count * route_count // experts_all
    slot_count = experts_all * capacity
    flat_ids = expert_index_table.reshape(seq_count * route_count)
    one_hot = (flat_ids[:, None] == jnp.arange(experts_all, dtype=jnp.int32)[None, :]).astype(
        jnp.int32
    )
    rank_in = jnp.sum(one_hot * (jnp.cumsum(one_hot, axis=0) - 1), axis=1)
    place_lookup = flat_ids * capacity + rank_in
    placing = (place_lookup[:, None] == jnp.arange(slot_count, dtype=jnp.int32)[None, :]).astype(
        jnp.float32
    )
    placing = placing.reshape(seq_count, route_count, slot_count)
    logit_exp = jnp.exp(expert_scores_within)
    weights = logit_exp / jnp.sum(logit_exp, axis=-1, keepdims=True) * group_probability[:, None]
    combine = jnp.einsum("sk,skc->sc", weights, placing, precision=lax.Precision.HIGHEST)
    dispatch = jnp.sum(placing, axis=1).astype(jnp.bfloat16)
    outgoing = jnp.einsum("sc,sd->cd", dispatch, normed_two, preferred_element_type=jnp.float32)
    outgoing = outgoing.astype(jnp.bfloat16).reshape(experts_all, capacity, model_width)
    width_local = expert_down_weight.shape[2]
    arrived = lax.all_to_all(outgoing, "ep", split_axis=0, concat_axis=0, tiled=True)
    held_slots = arrived.shape[1]
    grouped = arrived.reshape(ep_count, local_experts, held_slots, model_width)
    gate_pre = jnp.einsum(
        "sxcd,xfd->sxcf", grouped, expert_gate_weight, preferred_element_type=jnp.float32
    )
    up_pre = jnp.einsum(
        "sxcd,xfd->sxcf", grouped, expert_up_weight, preferred_element_type=jnp.float32
    )
    hidden = (jax.nn.silu(gate_pre) * up_pre).astype(jnp.bfloat16)
    outputs = jnp.einsum(
        "sxcf,xfd->sxcd",
        lax.all_gather(hidden, "tp", axis=3, tiled=True),
        expert_down_weight,
        preferred_element_type=jnp.float32,
    )
    ready_rows = outputs.astype(jnp.bfloat16).reshape(
        ep_count * local_experts, held_slots, width_local
    )
    returned = lax.all_to_all(ready_rows, "ep", split_axis=0, concat_axis=0, tiled=True)
    mixture = jnp.dot(
        combine,
        returned.reshape(slot_count, width_local).astype(jnp.float32),
        precision=lax.Precision.HIGHEST,
    )
    own_mixed = lax.dynamic_slice_in_dim(blended_tokens, tp_index * width_local, width_local, 1)
    new_stream = (own_mixed.astype(jnp.float32) + mixture).astype(jnp.bfloat16)
    return (new_stream, updated.reshape(seq_count, KEY_CHANNELS, value_local))


def f32(x):
    return x.astype(jnp.float32)


def bf16(x):
    return x.astype(jnp.bfloat16)


def exchange(x, axis, offset):
    size = lax.axis_size(axis)
    return lax.ppermute(x, axis, [(k, k ^ offset) for k in range(size)])


def project_kernel(tp_ref, *refs):
    piece_count = len(refs) - 7
    pieces = refs[:piece_count]
    gain, wq, wk, wv, wg, keep, send = refs[piece_count:]
    rows = pieces[0].shape[0] // CORES
    width = wq.shape[1]
    span = wv.shape[1]
    scaled = [bf16(f32(p[...]) * gain[...]) for p in pieces]
    x = jnp.concatenate(
        [p[:rows] for p in scaled] + [p[rows:] for p in scaled], axis=0
    )
    half = x.shape[0] // CORES
    start = 0
    for w in (wq, wk, wv, wg):
        y = jnp.dot(x, w[...], preferred_element_type=jnp.float32)
        keep[:, start : start + w.shape[1]] = bf16(y[:half])
        send[:, start : start + w.shape[1]] = bf16(y[half:])
        start += w.shape[1]


def project(tp_index, pieces, gain, wq, wk, wv, wg):
    heads = wv.shape[1] // DV
    features = wq.shape[0]
    rows = pieces[0].shape[0] * len(pieces) // CORES
    head_span = 2 * KEY_CHANNELS + 2 * DV
    own = lambda j, t: (0, t[0] * heads + j)
    local = lambda j, t: (0, j)
    whole = lambda j, t: (0, 0)
    out = jax.ShapeDtypeStruct((rows, heads * head_span), jnp.bfloat16)
    return pl.pallas_call(
        project_kernel,
        grid_spec=pltpu.PrefetchScalarGridSpec(
            num_scalar_prefetch=1,
            grid=(heads,),
            in_specs=[pl.BlockSpec(p.shape, whole) for p in pieces]
            + [
                pl.BlockSpec((1, features), whole),
                pl.BlockSpec((features, KEY_CHANNELS), own),
                pl.BlockSpec((features, KEY_CHANNELS), own),
                pl.BlockSpec((features, DV), local),
                pl.BlockSpec((features, DV), local),
            ],
            out_specs=[pl.BlockSpec((rows, head_span), local)] * 2,
        ),
        out_shape=[out, out],
        name="project",
    )(tp_index.reshape(1), *pieces, gain.reshape(1, features), wq, wk, wv, wg)


def as_columns(row, heads):
    parts = [row[:, h * KEY_CHANNELS : (h + 1) * KEY_CHANNELS] for h in range(heads)]
    pad = jnp.zeros((-heads % 8, KEY_CHANNELS), jnp.float32)
    return jnp.concatenate(parts + [pad], axis=0).T


def readout_kernel(*refs):
    piece_count = len(refs) - 12
    pieces = refs[:piece_count]
    (row_scale, decay, head_gain, state, gated, key_out, value_out, qd, qk, gate, read, _) = refs[
        piece_count:
    ]
    step = pl.program_id(0)
    heads = value_out.shape[1] // DV
    head_span = 2 * KEY_CHANNELS + 2 * DV
    per_step = state.shape[0]

    @pl.when(step == 0)
    def _():
        for h in range(heads):
            base = h * head_span
            total = f32(pieces[0][:, base : base + head_span])
            for p in pieces[1:]:
                total = total + f32(p[:, base : base + head_span])
            total = total * row_scale[...]
            q = f32(bf16(total[:, :KEY_CHANNELS] * KEY_CHANNELS ** (-0.5)))
            k = f32(bf16(total[:, KEY_CHANNELS : 2 * KEY_CHANNELS]))
            v = f32(bf16(total[:, 2 * KEY_CHANNELS : 2 * KEY_CHANNELS + DV]))
            g = f32(bf16(total[:, 2 * KEY_CHANNELS + DV :]))
            ks = slice(h * KEY_CHANNELS, (h + 1) * KEY_CHANNELS)
            vs = slice(h * DV, (h + 1) * DV)
            key_out[:, ks] = k
            value_out[:, vs] = v
            qd[:, ks] = q * decay[:, ks]
            qk[:, vs] = jnp.sum(q * k, axis=-1, keepdims=True) * v
            gate[:, vs] = g / (1.0 + jnp.exp(-g))

    for j in range(per_step):
        s = step * per_step + j
        cols = as_columns(qd[pl.ds(s, 1), :], heads)
        for h in range(heads):
            vs = slice(h * DV, (h + 1) * DV)
            prod = cols[:, h : h + 1] * state[j, :, vs]
            read[pl.ds(s, 1), vs] = jnp.sum(prod, axis=0, keepdims=True)

    @pl.when(step == pl.num_programs(0) - 1)
    def _():
        for h in range(heads):
            vs = slice(h * DV, (h + 1) * DV)
            r = read[:, vs] + qk[:, vs]
            inv = lax.rsqrt(jnp.mean(r * r, axis=-1, keepdims=True) + epsilon)
            gated[:, vs] = bf16(r * inv * head_gain[...] * gate[:, vs])


def readout_call(pieces, row_scale, decay, head_gain, state):
    seqs, channels, values = state.shape
    keys = decay.shape[1]
    per_step = 2
    whole = lambda i: (0, 0)
    full = lambda a: pl.BlockSpec(a.shape, whole)
    return pl.pallas_call(
        readout_kernel,
        grid=(seqs // per_step,),
        in_specs=[full(p) for p in pieces]
        + [full(row_scale), full(decay), full(head_gain)]
        + [pl.BlockSpec((per_step, channels, values), lambda i: (i, 0, 0))],
        out_specs=[
            pl.BlockSpec((seqs, values), whole),
            pl.BlockSpec((seqs, keys), whole),
            pl.BlockSpec((seqs, values), whole),
        ],
        out_shape=[
            jax.ShapeDtypeStruct((seqs, values), jnp.bfloat16),
            jax.ShapeDtypeStruct((seqs, keys), jnp.float32),
            jax.ShapeDtypeStruct((seqs, values), jnp.float32),
        ],
        scratch_shapes=[
            pltpu.VMEM((seqs, keys), jnp.float32),
            pltpu.VMEM((seqs, values), jnp.float32),
            pltpu.VMEM((seqs, values), jnp.float32),
            pltpu.VMEM((seqs, values), jnp.float32),
            pltpu.VMEM((8, 128), jnp.float32),
        ],
        name="readout",
    )(*pieces, row_scale, decay, head_gain, state)


def state_kernel(decay, keys, values, state, out):
    step = pl.program_id(0)
    per_step = state.shape[0]
    heads = values.shape[1] // DV
    for j in range(per_step):
        s = step * per_step + j
        decay_cols = as_columns(decay[pl.ds(s, 1), :], heads)
        key_cols = as_columns(keys[pl.ds(s, 1), :], heads)
        value_row = values[pl.ds(s, 1), :]
        for h in range(heads):
            vs = slice(h * DV, (h + 1) * DV)
            out[j, :, vs] = (
                decay_cols[:, h : h + 1] * state[j, :, vs]
                + key_cols[:, h : h + 1] * value_row[:, vs]
            )


def state_call(decay, keys, values, state):
    seqs, channels, width = state.shape
    per_step = 2
    block = pl.BlockSpec((per_step, channels, width), lambda i: (i, 0, 0))
    full = lambda a: pl.BlockSpec(a.shape, lambda i: (0, 0))
    return pl.pallas_call(
        state_kernel,
        grid=(seqs // per_step,),
        in_specs=[full(decay), full(keys), full(values), block],
        out_specs=block,
        out_shape=jax.ShapeDtypeStruct(state.shape, jnp.float32),
        cost_estimate=pl.CostEstimate(
            flops=40 * state.size, bytes_accessed=8 * state.size, transcendentals=0
        ),
        name="state_update",
    )(decay, keys, values, state)


def on_device_paired(
    stream,
    previous_state,
    mixer_norm_gain,
    query_matrix,
    key_matrix,
    value_matrix,
    output_gate_weight,
    decay_lower_factor,
    decay_upper_factor,
    forgetting_boost,
    head_norm_gain,
    output_matrix,
    mixture_norm_gain,
    expert_gate_weight,
    expert_up_weight,
    expert_down_weight,
    expert_index_table,
    expert_scores_within,
    group_probability,
):
    seq_count, model_width = stream.shape
    value_local = previous_state.shape[2]
    head_count = value_local // DV
    ep_count = lax.axis_size("ep")
    tp_count = lax.axis_size("tp")
    chips = ep_count // CORES
    tp_index = lax.axis_index("tp")
    ep_index = lax.axis_index("ep")
    chip, core = ep_index // CORES, ep_index % CORES
    key_column_span = head_count * KEY_CHANNELS
    first_key = tp_index * key_column_span
    features = query_matrix.shape[0]

    partner_stream = exchange(stream, "ep", 1)
    pieces = []
    for d in range(chips):
        start = ((chip ^ d) * CORES + core) * features
        both = [lax.dynamic_slice_in_dim(a, start, features, 1) for a in (stream, partner_stream)]
        block = jnp.concatenate(both, axis=0)
        pieces.append(exchange(block, "ep", CORES * d) if d else block)
    own_gain = lax.dynamic_slice_in_dim(mixer_norm_gain, ep_index * features, features, 0)
    keep, send = project(
        tp_index, pieces, own_gain, query_matrix, key_matrix, value_matrix, output_gate_weight
    )
    on_chip = bf16(f32(keep) + f32(exchange(send, "ep", 1)))
    sums = []
    for d in range(chips):
        block = on_chip[d * seq_count : (d + 1) * seq_count]
        sums.append(exchange(block, "ep", CORES * d) if d else block)

    floats = f32(stream)
    row_scale = lax.rsqrt(jnp.mean(floats * floats, axis=-1, keepdims=True) + epsilon)
    normed = bf16(floats * row_scale * mixer_norm_gain)
    low_rank = bf16(jnp.dot(normed, decay_lower_factor, preferred_element_type=jnp.float32))
    local_upper = lax.dynamic_slice_in_dim(decay_upper_factor, first_key, key_column_span, 1)
    logit = jnp.dot(low_rank, local_upper, preferred_element_type=jnp.float32)
    boost = lax.dynamic_slice_in_dim(forgetting_boost, first_key, key_column_span, 1)
    decay = jnp.exp(jax.nn.log_sigmoid(logit) / forgetting_softness - boost)

    gated_rows, key_rows, value_rows = readout_call(
        sums, row_scale, decay, head_norm_gain.reshape(1, DV), previous_state
    )
    partial_out = bf16(jnp.dot(gated_rows, output_matrix, preferred_element_type=jnp.float32))
    mixed = floats + f32(partial_out)
    for d in range(1, tp_count):
        mixed = mixed + f32(exchange(partial_out, "tp", d))
    new_state = state_call(decay, key_rows, value_rows, previous_state)
    mixed = bf16(mixed)
    normed_two = rms_scaled(mixed, mixture_norm_gain)

    route_count = expert_index_table.shape[1]
    capacity = 2 * seq_count * route_count // (ep_count * expert_gate_weight.shape[0])
    slot_count = chips * capacity
    relative = (expert_index_table[:, 0] // CORES) ^ chip
    in_group = (relative[:, None] == jnp.arange(chips, dtype=jnp.int32)[None, :]).astype(jnp.int32)
    earlier = (
        jnp.arange(seq_count, dtype=jnp.int32)[:, None]
        > jnp.arange(seq_count, dtype=jnp.int32)[None, :]
    )
    same = relative[:, None] == relative[None, :]
    rank = jnp.sum((earlier & same).astype(jnp.int32), axis=1)
    place = relative * capacity + rank
    placing = place[:, None] == jnp.arange(slot_count, dtype=jnp.int32)[None, :]
    logit_exp = jnp.exp(expert_scores_within)
    weights = logit_exp / jnp.sum(logit_exp, axis=-1, keepdims=True) * group_probability[:, None]
    at_core = expert_index_table % CORES
    combine = jnp.stack(
        [
            jnp.where(
                placing,
                jnp.sum(jnp.where(at_core == which, weights, 0.0), axis=1, keepdims=True),
                0.0,
            ).reshape(seq_count, chips, capacity)
            for which in (core, 1 - core)
        ],
        axis=2,
    ).reshape(seq_count, CORES * slot_count)
    outgoing = bf16(
        jnp.einsum(
            "sc,sd->cd", bf16(placing), normed_two, preferred_element_type=jnp.float32
        )
    )
    arrived = []
    for d in range(chips):
        block = outgoing[d * capacity : (d + 1) * capacity]
        arrived.append(exchange(block, "ep", CORES * d) if d else block)
    arrived = jnp.concatenate(arrived, axis=0)
    rows = jnp.concatenate([arrived, exchange(arrived, "ep", 1)], axis=0)

    contract_last = (((1,), (1,)), ((), ()))
    gate_pre = lax.dot_general(
        rows, expert_gate_weight[0], contract_last, preferred_element_type=jnp.float32
    )
    up_pre = lax.dot_general(
        rows, expert_up_weight[0], contract_last, preferred_element_type=jnp.float32
    )
    hidden = bf16(jax.nn.silu(gate_pre) * up_pre)
    parts = jnp.stack([hidden] + [exchange(hidden, "tp", d) for d in range(1, tp_count)])
    hidden_all = jnp.concatenate(
        [
            lax.dynamic_index_in_dim(parts, tp_index ^ j, 0, keepdims=False)
            for j in range(tp_count)
        ],
        axis=1,
    )
    outputs = bf16(
        jnp.dot(hidden_all, expert_down_weight[0], preferred_element_type=jnp.float32)
    )
    width_local = outputs.shape[1]
    same_core = outputs[:slot_count].reshape(chips, capacity, width_local)
    other_core = exchange(outputs[slot_count:], "ep", 1).reshape(chips, capacity, width_local)
    back = []
    for d in range(chips):
        block = jnp.concatenate([same_core[d], other_core[d]], axis=0)
        back.append(exchange(block, "ep", CORES * d) if d else block)
    mixture = jnp.dot(
        combine, f32(jnp.concatenate(back, axis=0)), precision=lax.Precision.HIGHEST
    )
    own_mixed = lax.dynamic_slice_in_dim(mixed, tp_index * width_local, width_local, 1)
    new_stream = bf16(f32(own_mixed) + mixture)
    return (new_stream, new_state)


def power_of_two(n):
    return n & (n - 1) == 0


def on_device(*args):
    values, local_experts = args[1].shape[2], args[13].shape[0]
    ep_count, tp_count = lax.axis_size("ep"), lax.axis_size("tp")
    per_group = ep_count * local_experts // GROUPS
    paired = (
        values % DV == 0
        and local_experts == 1
        and per_group == CORES
        and args[16].shape[1] == CORES
        and power_of_two(ep_count)
        and power_of_two(tp_count)
    )
    return (on_device_paired if paired else on_device_general)(*args)


def solution(mesh):
    placed = (
        P("ep", None),
        P("ep", None, "tp"),
        P(),
        P("ep", None),
        P("ep", None),
        P("ep", "tp"),
        P("ep", "tp"),
        P(),
        P(),
        P("ep", None),
        P(),
        P("tp", None),
        P(),
        P("ep", "tp", None),
        P("ep", "tp", None),
        P("ep", None, "tp"),
        P("ep", None),
        P("ep", None),
        P("ep"),
    )
    return jax.shard_map(
        on_device,
        mesh=mesh,
        in_specs=placed,
        out_specs=(P("ep", "tp"), P("ep", None, "tp")),
        check_vma=False,
    )
```

```python
import jax
import jax.numpy as jnp
from jax import lax
from jax.experimental import pallas as pl
from jax.experimental.pallas import tpu as pltpu
from jax.sharding import PartitionSpec as P

HEAD_TOTAL = 16
KEY_CHANNELS = 128
DV = 256
GROUPS = 4
CORES = 2


epsilon = 1e-06
forgetting_softness = 16.0


def rms_scaled(values, gain_vec):
    floats = values.astype(jnp.float32)
    scaled = floats * lax.rsqrt(jnp.mean(floats * floats, axis=-1, keepdims=True) + epsilon)
    return (scaled * gain_vec).astype(jnp.bfloat16)


def on_device_general(
    stream,
    previous_state,
    mixer_norm_gain,
    query_matrix,
    key_matrix,
    value_matrix,
    output_gate_weight,
    decay_lower_factor,
    decay_upper_factor,
    forgetting_boost,
    head_norm_gain,
    output_matrix,
    mixture_norm_gain,
    expert_gate_weight,
    expert_up_weight,
    expert_down_weight,
    expert_index_table,
    expert_scores_within,
    group_probability,
):
    seq_count, model_width = stream.shape
    value_local = previous_state.shape[2]
    head_count = max(1, value_local // DV)
    head_width = min(value_local, DV)
    tp_index = lax.axis_index("tp")
    leading_head = tp_index * value_local // DV
    value_start = tp_index * value_local % DV
    key_column_span = head_count * KEY_CHANNELS
    normed = rms_scaled(stream, mixer_norm_gain)
    own_query = lax.dynamic_slice_in_dim(
        query_matrix, leading_head * KEY_CHANNELS, key_column_span, 1
    )
    own_key = lax.dynamic_slice_in_dim(key_matrix, leading_head * KEY_CHANNELS, key_column_span, 1)
    spread = lax.all_to_all(normed, "ep", split_axis=1, concat_axis=0, tiled=True)
    joined = jnp.concatenate([own_query, own_key, value_matrix, output_gate_weight], axis=1)
    summed = lax.psum_scatter(
        jnp.dot(spread, joined, preferred_element_type=jnp.float32),
        "ep",
        scatter_dimension=0,
        tiled=True,
    )
    query_sum = summed[:, :key_column_span]
    key_sum = summed[:, key_column_span : 2 * key_column_span]
    value_sum = summed[:, 2 * key_column_span : 2 * key_column_span + value_local]
    gate_sum = summed[:, 2 * key_column_span + value_local :]
    queries = (query_sum * KEY_CHANNELS ** (-0.5)).astype(jnp.bfloat16)
    key_rows = key_sum.astype(jnp.bfloat16)
    value_rows = value_sum.astype(jnp.bfloat16)
    gate_rows = gate_sum.astype(jnp.bfloat16)
    low_rank = jnp.dot(normed, decay_lower_factor, preferred_element_type=jnp.float32).astype(
        jnp.bfloat16
    )
    local_expand_matrix = lax.dynamic_slice_in_dim(
        decay_upper_factor, leading_head * KEY_CHANNELS, key_column_span, 1
    )
    forgetting_logit = jnp.dot(low_rank, local_expand_matrix, preferred_element_type=jnp.float32)
    request_boost = lax.dynamic_slice_in_dim(
        forgetting_boost, leading_head * KEY_CHANNELS, key_column_span, 1
    )
    forgetting_lograte = jax.nn.log_sigmoid(forgetting_logit) / forgetting_softness - request_boost
    factor = (
        jnp.exp(forgetting_lograte)
        .reshape(seq_count, head_count, KEY_CHANNELS)
        .transpose(0, 2, 1)[..., None]
    )
    state_four = previous_state.reshape(seq_count, KEY_CHANNELS, head_count, head_width)
    key_part = (
        key_rows.astype(jnp.float32)
        .reshape(seq_count, head_count, KEY_CHANNELS)
        .transpose(0, 2, 1)[..., None]
    )
    value_part = value_rows.astype(jnp.float32).reshape(seq_count, 1, head_count, head_width)
    updated = factor * state_four + key_part * value_part
    query_part = (
        queries.astype(jnp.float32).reshape(seq_count, head_count, KEY_CHANNELS).transpose(0, 2, 1)
    )
    readout = jnp.einsum("skh,skhv->shv", query_part, updated, precision=lax.Precision.HIGHEST)
    square_sums = jnp.sum(readout * readout, axis=-1)
    norm_table = lax.dynamic_update_slice(
        jnp.zeros((seq_count, HEAD_TOTAL), jnp.float32), square_sums, (jnp.int32(0), leading_head)
    )
    totals = lax.psum(norm_table, "tp")
    own_totals = lax.dynamic_slice_in_dim(totals, leading_head, head_count, 1)
    mean_sq = own_totals[..., None] / DV
    own_gain = lax.dynamic_slice_in_dim(head_norm_gain, value_start, head_width, 0)
    gate_part = jax.nn.silu(
        gate_rows.astype(jnp.float32).reshape(seq_count, head_count, head_width)
    )
    gated_rows = (
        (readout * lax.rsqrt(mean_sq + epsilon) * own_gain * gate_part)
        .reshape(seq_count, value_local)
        .astype(jnp.bfloat16)
    )
    partial_out = jnp.dot(gated_rows, output_matrix, preferred_element_type=jnp.float32)
    mixer_sum = lax.psum(partial_out.astype(jnp.bfloat16), "tp").astype(jnp.float32)
    blended_tokens = (stream.astype(jnp.float32) + mixer_sum).astype(jnp.bfloat16)
    normed_two = rms_scaled(blended_tokens, mixture_norm_gain)
    ep_count = lax.axis_size("ep")
    local_experts = expert_gate_weight.shape[0]
    experts_all = ep_count * local_experts
    route_count = expert_index_table.shape[1]
    capacity = 2 * seq_count * route_count // experts_all
    slot_count = experts_all * capacity
    flat_ids = expert_index_table.reshape(seq_count * route_count)
    one_hot = (flat_ids[:, None] == jnp.arange(experts_all, dtype=jnp.int32)[None, :]).astype(
        jnp.int32
    )
    rank_in = jnp.sum(one_hot * (jnp.cumsum(one_hot, axis=0) - 1), axis=1)
    place_lookup = flat_ids * capacity + rank_in
    placing = (place_lookup[:, None] == jnp.arange(slot_count, dtype=jnp.int32)[None, :]).astype(
        jnp.float32
    )
    placing = placing.reshape(seq_count, route_count, slot_count)
    logit_exp = jnp.exp(expert_scores_within)
    weights = logit_exp / jnp.sum(logit_exp, axis=-1, keepdims=True) * group_probability[:, None]
    combine = jnp.einsum("sk,skc->sc", weights, placing, precision=lax.Precision.HIGHEST)
    dispatch = jnp.sum(placing, axis=1).astype(jnp.bfloat16)
    outgoing = jnp.einsum("sc,sd->cd", dispatch, normed_two, preferred_element_type=jnp.float32)
    outgoing = outgoing.astype(jnp.bfloat16).reshape(experts_all, capacity, model_width)
    width_local = expert_down_weight.shape[2]
    arrived = lax.all_to_all(outgoing, "ep", split_axis=0, concat_axis=0, tiled=True)
    held_slots = arrived.shape[1]
    grouped = arrived.reshape(ep_count, local_experts, held_slots, model_width)
    gate_pre = jnp.einsum(
        "sxcd,xfd->sxcf", grouped, expert_gate_weight, preferred_element_type=jnp.float32
    )
    up_pre = jnp.einsum(
        "sxcd,xfd->sxcf", grouped, expert_up_weight, preferred_element_type=jnp.float32
    )
    hidden = (jax.nn.silu(gate_pre) * up_pre).astype(jnp.bfloat16)
    outputs = jnp.einsum(
        "sxcf,xfd->sxcd",
        lax.all_gather(hidden, "tp", axis=3, tiled=True),
        expert_down_weight,
        preferred_element_type=jnp.float32,
    )
    ready_rows = outputs.astype(jnp.bfloat16).reshape(
        ep_count * local_experts, held_slots, width_local
    )
    returned = lax.all_to_all(ready_rows, "ep", split_axis=0, concat_axis=0, tiled=True)
    mixture = jnp.dot(
        combine,
        returned.reshape(slot_count, width_local).astype(jnp.float32),
        precision=lax.Precision.HIGHEST,
    )
    own_mixed = lax.dynamic_slice_in_dim(blended_tokens, tp_index * width_local, width_local, 1)
    new_stream = (own_mixed.astype(jnp.float32) + mixture).astype(jnp.bfloat16)
    return (new_stream, updated.reshape(seq_count, KEY_CHANNELS, value_local))


def f32(x):
    return x.astype(jnp.float32)


def bf16(x):
    return x.astype(jnp.bfloat16)


def exchange(x, axis, offset):
    size = lax.axis_size(axis)
    return lax.ppermute(x, axis, [(k, k ^ offset) for k in range(size)])


IN_VMEM = pl.BlockSpec(memory_space=pltpu.VMEM)


def small_kernel(**more):
    return pltpu.CompilerParams(vmem_limit_bytes=8 * 2**20, **more)


def project_kernel(*refs):
    piece_count = len(refs) - 7
    pieces = refs[:piece_count]
    gain, wq, wk, wv, wg, keep, send = refs[piece_count:]
    rows = pieces[0].shape[0] // CORES
    scaled = [bf16(f32(p[...]) * gain[...]) for p in pieces]
    x = jnp.concatenate(
        [p[:rows] for p in scaled] + [p[rows:] for p in scaled], axis=0
    )
    half = x.shape[0] // CORES
    start = 0
    for w in (wq, wk, wv, wg):
        y = jnp.dot(x, w[...], preferred_element_type=jnp.float32)
        keep[:, start : start + w.shape[1]] = bf16(y[:half])
        send[:, start : start + w.shape[1]] = bf16(y[half:])
        start += w.shape[1]


def project(pieces, gain, wq, wk, wv, wg):
    rows = pieces[0].shape[0] * len(pieces) // CORES
    out = jax.ShapeDtypeStruct((rows, 2 * (wq.shape[1] + wv.shape[1])), jnp.bfloat16)
    return pl.pallas_call(
        project_kernel,
        in_specs=[IN_VMEM] * (len(pieces) + 5),
        out_specs=[IN_VMEM] * 2,
        out_shape=[out, out],
        compiler_params=small_kernel(),
        name="project",
    )(*pieces, gain.reshape(1, -1), wq, wk, wv, wg)


def as_columns(row, heads):
    parts = [row[:, h * KEY_CHANNELS : (h + 1) * KEY_CHANNELS] for h in range(heads)]
    pad = jnp.zeros((-heads % 8, KEY_CHANNELS), jnp.float32)
    return jnp.concatenate(parts + [pad], axis=0).T


def readout_kernel(*refs):
    piece_count = len(refs) - 13
    pieces = refs[:piece_count]
    (row_scale, decay, head_gain, state, w_out, partial, key_out, value_out) = refs[
        piece_count : piece_count + 8
    ]
    qd, qk, gate, read, gated = refs[piece_count + 8 :]
    seqs, values = value_out.shape
    heads = values // DV
    keys = key_out.shape[1]

    def summed(start, width):
        total = f32(pieces[0][:, start : start + width])
        for p in pieces[1:]:
            total = total + f32(p[:, start : start + width])
        return total * row_scale[...]

    for h in range(heads):
        ks = slice(h * KEY_CHANNELS, (h + 1) * KEY_CHANNELS)
        vs = slice(h * DV, (h + 1) * DV)
        q = f32(bf16(summed(h * KEY_CHANNELS, KEY_CHANNELS) * KEY_CHANNELS ** (-0.5)))
        k = f32(bf16(summed(keys + h * KEY_CHANNELS, KEY_CHANNELS)))
        v = f32(bf16(summed(2 * keys + h * DV, DV)))
        g = f32(bf16(summed(2 * keys + values + h * DV, DV)))
        key_out[:, ks] = k
        value_out[:, vs] = v
        qd[:, ks] = q * decay[:, ks]
        qk[:, vs] = jnp.sum(q * k, axis=-1, keepdims=True) * v
        gate[:, vs] = g / (1.0 + jnp.exp(-g))

    def body(s, carry):
        cols = as_columns(qd[pl.ds(s, 1), :], heads)
        for h in range(heads):
            vs = slice(h * DV, (h + 1) * DV)
            col = cols[:, h : h + 1]
            acc = jnp.zeros((8, DV), jnp.float32)
            for i in range(0, KEY_CHANNELS, 8):
                acc = acc + col[i : i + 8] * state[s, i : i + 8, vs]
            read[pl.ds(s, 1), vs] = jnp.sum(acc, axis=0, keepdims=True)
        return carry

    lax.fori_loop(0, seqs, body, 0, unroll=4)
    for h in range(heads):
        vs = slice(h * DV, (h + 1) * DV)
        r = read[:, vs] + qk[:, vs]
        inv = lax.rsqrt(jnp.mean(r * r, axis=-1, keepdims=True) + epsilon)
        gated[:, vs] = bf16(r * inv * head_gain[...] * gate[:, vs])
    partial[...] = bf16(
        jnp.dot(gated[...], w_out[...], preferred_element_type=jnp.float32)
    )


def readout_call(pieces, row_scale, decay, head_gain, state, w_out):
    seqs, channels, values = state.shape
    keys = decay.shape[1]
    return pl.pallas_call(
        readout_kernel,
        in_specs=[IN_VMEM] * (len(pieces) + 5),
        out_specs=[IN_VMEM] * 3,
        out_shape=[
            jax.ShapeDtypeStruct((seqs, w_out.shape[1]), jnp.bfloat16),
            jax.ShapeDtypeStruct((seqs, keys), jnp.float32),
            jax.ShapeDtypeStruct((seqs, values), jnp.float32),
        ],
        scratch_shapes=[
            pltpu.VMEM((seqs, keys), jnp.float32),
            pltpu.VMEM((seqs, values), jnp.float32),
            pltpu.VMEM((seqs, values), jnp.float32),
            pltpu.VMEM((seqs, values), jnp.float32),
            pltpu.VMEM((seqs, values), jnp.bfloat16),
        ],
        compiler_params=small_kernel(),
        name="readout",
    )(*pieces, row_scale, decay, head_gain, state, w_out)


def state_kernel(first, decay, keys, values, state, *rest):
    out = rest[-1]
    s = first + pl.program_id(0)
    heads = values.shape[1] // DV
    decay_cols = as_columns(decay[pl.ds(s, 1), :], heads)
    key_cols = as_columns(keys[pl.ds(s, 1), :], heads)
    value_row = values[pl.ds(s, 1), :]
    for h in range(heads):
        vs = slice(h * DV, (h + 1) * DV)
        out[0, :, vs] = (
            decay_cols[:, h : h + 1] * state[0, :, vs]
            + key_cols[:, h : h + 1] * value_row[:, vs]
        )


def state_call(first, count, decay, keys, values, state, earlier):
    seqs, channels, width = state.shape
    block = pl.BlockSpec((1, channels, width), lambda i: (first + i, 0, 0))
    full = lambda a: pl.BlockSpec(a.shape, lambda i: (0, 0))
    kept = () if earlier is None else (earlier,)
    return pl.pallas_call(
        lambda *refs: state_kernel(first, *refs),
        grid=(count,),
        in_specs=[full(decay), full(keys), full(values), block]
        + [pl.BlockSpec(memory_space=pl.ANY)] * len(kept),
        out_specs=block,
        out_shape=jax.ShapeDtypeStruct(state.shape, jnp.float32),
        input_output_aliases={4: 0} if kept else {},
        compiler_params=small_kernel(),
        cost_estimate=pl.CostEstimate(
            flops=40 * count * channels * width,
            bytes_accessed=8 * count * channels * width,
            transcendentals=0,
        ),
        name="state_update",
    )(decay, keys, values, pltpu.with_memory_space_constraint(state, pltpu.HBM), *kept)


def on_device_paired(
    stream,
    previous_state,
    mixer_norm_gain,
    query_matrix,
    key_matrix,
    value_matrix,
    output_gate_weight,
    decay_lower_factor,
    decay_upper_factor,
    forgetting_boost,
    head_norm_gain,
    output_matrix,
    mixture_norm_gain,
    expert_gate_weight,
    expert_up_weight,
    expert_down_weight,
    expert_index_table,
    expert_scores_within,
    group_probability,
):
    seq_count, model_width = stream.shape
    value_local = previous_state.shape[2]
    head_count = value_local // DV
    ep_count = lax.axis_size("ep")
    tp_count = lax.axis_size("tp")
    chips = ep_count // CORES
    tp_index = lax.axis_index("tp")
    ep_index = lax.axis_index("ep")
    chip, core = ep_index // CORES, ep_index % CORES
    key_column_span = head_count * KEY_CHANNELS
    first_key = tp_index * key_column_span
    features = query_matrix.shape[0]

    partner_stream = exchange(stream, "ep", 1)
    blocks = []
    for d in range(chips):
        start = ((chip ^ d) * CORES + core) * features
        both = [lax.dynamic_slice_in_dim(a, start, features, 1) for a in (stream, partner_stream)]
        blocks.append(jnp.concatenate(both, axis=0))
    pieces = [exchange(block, "ep", CORES * d) if d else block for d, block in enumerate(blocks)]
    own_gain = lax.dynamic_slice_in_dim(mixer_norm_gain, ep_index * features, features, 0)
    own_query, own_key = [
        lax.dynamic_slice_in_dim(w, first_key, key_column_span, 1)
        for w in (query_matrix, key_matrix)
    ]
    keep, send = project(pieces, own_gain, own_query, own_key, value_matrix, output_gate_weight)
    on_chip = bf16(f32(keep) + f32(exchange(send, "ep", 1)))
    sums = []
    for d in range(chips):
        block = on_chip[d * seq_count : (d + 1) * seq_count]
        sums.append(exchange(block, "ep", CORES * d) if d else block)

    floats = f32(stream)
    row_scale = lax.rsqrt(jnp.mean(floats * floats, axis=-1, keepdims=True) + epsilon)
    normed = bf16(floats * row_scale * mixer_norm_gain)
    low_rank = bf16(jnp.dot(normed, decay_lower_factor, preferred_element_type=jnp.float32))
    local_upper = lax.dynamic_slice_in_dim(decay_upper_factor, first_key, key_column_span, 1)
    logit = jnp.dot(low_rank, local_upper, preferred_element_type=jnp.float32)
    boost = lax.dynamic_slice_in_dim(forgetting_boost, first_key, key_column_span, 1)
    decay = jnp.exp(jax.nn.log_sigmoid(logit) / forgetting_softness - boost)

    partial_out, key_rows, value_rows = readout_call(
        sums, row_scale, decay, head_norm_gain.reshape(1, DV), previous_state, output_matrix
    )
    bounds = [seq_count * n // 16 for n in (0, 5, 9, 12, 16)]

    def update(n, earlier, after):
        held, _ = lax.optimization_barrier((decay, after))
        return state_call(
            bounds[n], bounds[n + 1] - bounds[n], held, key_rows, value_rows, previous_state, earlier
        )

    mixed = floats + f32(partial_out)
    for d in range(1, tp_count):
        mixed = mixed + f32(exchange(partial_out, "tp", d))
    new_state = update(0, None, partial_out)
    mixed = bf16(mixed)
    normed_two = rms_scaled(mixed, mixture_norm_gain)

    route_count = expert_index_table.shape[1]
    capacity = 2 * seq_count * route_count // (ep_count * expert_gate_weight.shape[0])
    slot_count = chips * capacity
    relative = (expert_index_table[:, 0] // CORES) ^ chip
    in_group = (relative[:, None] == jnp.arange(chips, dtype=jnp.int32)[None, :]).astype(jnp.int32)
    earlier = (
        jnp.arange(seq_count, dtype=jnp.int32)[:, None]
        > jnp.arange(seq_count, dtype=jnp.int32)[None, :]
    )
    same = relative[:, None] == relative[None, :]
    rank = jnp.sum((earlier & same).astype(jnp.int32), axis=1)
    place = relative * capacity + rank
    placing = place[:, None] == jnp.arange(slot_count, dtype=jnp.int32)[None, :]
    logit_exp = jnp.exp(expert_scores_within)
    weights = logit_exp / jnp.sum(logit_exp, axis=-1, keepdims=True) * group_probability[:, None]
    at_core = expert_index_table % CORES
    combine = jnp.stack(
        [
            jnp.where(
                placing,
                jnp.sum(jnp.where(at_core == which, weights, 0.0), axis=1, keepdims=True),
                0.0,
            ).reshape(seq_count, chips, capacity)
            for which in (core, 1 - core)
        ],
        axis=2,
    ).reshape(seq_count, CORES * slot_count)
    outgoing = bf16(
        jnp.einsum(
            "sc,sd->cd", bf16(placing), normed_two, preferred_element_type=jnp.float32
        )
    )
    outgoing, new_state = lax.optimization_barrier((outgoing, new_state))
    new_state = update(1, new_state, outgoing)
    arrived = []
    for d in range(chips):
        block = outgoing[d * capacity : (d + 1) * capacity]
        arrived.append(exchange(block, "ep", CORES * d) if d else block)
    arrived = jnp.concatenate(arrived, axis=0)
    rows = jnp.concatenate([arrived, exchange(arrived, "ep", 1)], axis=0)

    contract_last = (((1,), (1,)), ((), ()))
    gate_pre = lax.dot_general(
        rows, expert_gate_weight[0], contract_last, preferred_element_type=jnp.float32
    )
    up_pre = lax.dot_general(
        rows, expert_up_weight[0], contract_last, preferred_element_type=jnp.float32
    )
    hidden = bf16(jax.nn.silu(gate_pre) * up_pre)
    hidden, new_state = lax.optimization_barrier((hidden, new_state))
    new_state = update(2, new_state, hidden)
    parts = jnp.stack([hidden] + [exchange(hidden, "tp", d) for d in range(1, tp_count)])
    hidden_all = jnp.concatenate(
        [
            lax.dynamic_index_in_dim(parts, tp_index ^ j, 0, keepdims=False)
            for j in range(tp_count)
        ],
        axis=1,
    )
    outputs = bf16(
        jnp.dot(hidden_all, expert_down_weight[0], preferred_element_type=jnp.float32)
    )
    outputs, new_state = lax.optimization_barrier((outputs, new_state))
    width_local = outputs.shape[1]
    same_core = outputs[:slot_count].reshape(chips, capacity, width_local)
    other_core = exchange(outputs[slot_count:], "ep", 1)
    new_state = update(3, new_state, other_core)
    other_core = other_core.reshape(chips, capacity, width_local)
    back = []
    for d in range(chips):
        block = jnp.concatenate([same_core[d], other_core[d]], axis=0)
        back.append(exchange(block, "ep", CORES * d) if d else block)
    mixture = jnp.dot(
        combine, f32(jnp.concatenate(back, axis=0)), precision=lax.Precision.HIGHEST
    )
    own_mixed = lax.dynamic_slice_in_dim(mixed, tp_index * width_local, width_local, 1)
    new_stream = bf16(f32(own_mixed) + mixture)
    return (new_stream, new_state)


def power_of_two(n):
    return n & (n - 1) == 0


def on_device(*args):
    values, local_experts = args[1].shape[2], args[13].shape[0]
    ep_count, tp_count = lax.axis_size("ep"), lax.axis_size("tp")
    per_group = ep_count * local_experts // GROUPS
    paired = (
        values % DV == 0
        and local_experts == 1
        and per_group == CORES
        and args[16].shape[1] == CORES
        and power_of_two(ep_count)
        and power_of_two(tp_count)
    )
    return (on_device_paired if paired else on_device_general)(*args)


def solution(mesh):
    placed = (
        P("ep", None),
        P("ep", None, "tp"),
        P(),
        P("ep", None),
        P("ep", None),
        P("ep", "tp"),
        P("ep", "tp"),
        P(),
        P(),
        P("ep", None),
        P(),
        P("tp", None),
        P(),
        P("ep", "tp", None),
        P("ep", "tp", None),
        P("ep", None, "tp"),
        P("ep", None),
        P("ep", None),
        P("ep"),
    )
    return jax.shard_map(
        on_device,
        mesh=mesh,
        in_specs=placed,
        out_specs=(P("ep", "tp"), P("ep", None, "tp")),
        check_vma=False,
    )
```
